32 devices in a mesh: sp: 8 (over z, core), tp: 4 (over y, x).
Axes of the slice: x: 2, y: 2, z: 4, core: 2. Of those that a mesh axis runs over, the one named last changes fastest.
Arguments:
- residual_in: bfloat16 [2048, 2048], P('sp'), may hold values from -3 to 3
- mix_gain: float32 [2048], replicated, may hold values from 0.1 to 1.9
- pool_weight: bfloat16 [512, 2048], P(None, 'tp'), may hold values from -0.5 to 0.5
- pool_scale: float32 [2048], P('tp'), may hold values from 0.1 to 1.9
- ffn_gain: float32 [2048], replicated, may hold values from 0.1 to 1.9
- route_ids: int32 [2048, 2], P('sp'), may hold values from 0 to 7, all different within a row; in each aligned block of 64 rows (0 to 63, 64 to 127, ...) at most 32 rows name the same one
- route_weights: float32 [2048, 2], P('sp'), may hold values from 0.1 to 1
- gate_weight: bfloat16 [8, 2048, 3584], P('sp', None, 'tp'), may hold values from -0.125 to 0.125
- up_weight: bfloat16 [8, 2048, 3584], P('sp', None, 'tp'), may hold values from -0.125 to 0.125
- down_weight: bfloat16 [8, 3584, 2048], P('sp', 'tp'), may hold values from -0.09375 to 0.09375
Outputs:
- layer_out: bfloat16 [2048, 2048], P('sp')
The draws below stay inside these ranges and needn't reach their ends.
Inputs may be any that keep to these rules, and one draw needn't show every extreme that they name: `route_ids`: each row names 2 different experts; in each aligned block of 64 rows no expert is named by more than 32 rows, and some block has an expert named by exactly 32 rows.
All inputs are finite; a program needn't handle non-finite values.
Results may differ from the reference program's by a relative error of at most 0.0074.
Values may be sent and summed in bfloat16 or wider, within the bound.
A program may use at most 64 MiB of HBM per device.

```python
import math
import jax
import jax.numpy as jnp
import numpy as np
from jax import lax

D = 2048
GROUPS = 4
SPAN = 16
C = 512
FF_EXP = 3584
TOP_K = 2
EXPERTS = 8
ROWS = 64
CAP = 32
TOKENS = 2048
N_TP = 4


def level_of(rng, shape, split, smallest, top_value):
    def one(dim, parts):
        draws = jax.random.uniform(jax.random.fold_in(jax.random.fold_in(rng, 6), dim), (parts,), jnp.float32, smallest / len(split), top_value / len(split))
        return jnp.repeat(jnp.exp(draws), shape[dim] // parts).reshape((-1,) + (1,) * (len(shape) - dim - 1))

    factor_of = one(*split[0])
    for cut in split[1:]:
        factor_of = factor_of * one(*cut)
    return factor_of


def deal_out(key, own, number, rows, number_of, top, most, lean):
    sequence = jax.random.permutation(key, number_of)
    heavy_load, ordinary = shares(number_of, rows * top, most, lean, True), shares(number_of, rows * top, most, lean, False)
    places = jnp.arange(number_of)

    def named(sizes, offset_by):
        used = int((sizes > 0).sum())
        fixed = max(1, used // 4)
        passed = fixed + (places - fixed + offset_by * (used - fixed)) % max(1, number_of - fixed)
        return jnp.zeros((number_of,), jnp.int32).at[sequence[jnp.where(places < fixed, places, passed)]].set(jnp.asarray(sizes, jnp.int32))

    sizes = jnp.where(number % 4 == 0, named(heavy_load, number // 4), named(ordinary, number - number // 4 - 1))
    mixed = jax.random.permutation(jax.random.fold_in(own, 3), number_of)
    source_of, receiver = mixed[0:number_of // 2 * 2:2], mixed[1:number_of // 2 * 2:2]
    room = jnp.minimum(sizes[source_of] - 1, most - sizes[receiver]) // 2
    room = jnp.where((source_of == sequence[0]) | (receiver == sequence[0]) | (sizes[receiver] == 0), 0, jnp.maximum(room, 0))
    passed = jax.random.randint(jax.random.fold_in(own, 4), (number_of // 2,), 0, 1 << 20) % (room + 1)
    sizes = sizes.at[source_of].add(-passed).at[receiver].add(passed)
    items = jnp.searchsorted(jnp.cumsum(sizes), jnp.arange(rows * top), side="right").astype(jnp.int32)
    table = items.reshape(top, rows).T
    table = table[jax.random.permutation(jax.random.fold_in(own, 1), rows)]
    offset_by = jax.random.randint(jax.random.fold_in(own, 2), (rows, 1), 0, top)
    return jnp.take_along_axis(table, (jnp.arange(top)[None, :] + offset_by) % top, axis=1)


def shares(number_of, total, bound, lean, full):
    loads = [(1 << 20) // math.isqrt(standing ** lean) + 1 for standing in range(1, number_of + 1)]
    largest = bound if full else min(bound, max(-(-total // number_of), total * loads[0] // sum(loads)))
    least = 1 if total - largest >= number_of - 1 else 0
    counts, surplus = [largest] + [least] * (number_of - 1), total - largest - least * (number_of - 1)
    while surplus > 0:
        movable = [i for i in range(1, number_of) if counts[i] < largest] or [i for i in range(1, number_of) if counts[i] < bound]
        pool, remaining = sum([loads[i] for i in movable]), surplus
        for i in movable:
            extra = min(bound - counts[i], max(1, remaining * loads[i] // pool), surplus)
            counts[i] = counts[i] + extra
            surplus = surplus - extra
    return np.array(counts)


def gaussian(stream_key, shape, deviation, most, cuts=(), held_as=jnp.bfloat16):
    result = jax.random.normal(stream_key, shape, jnp.float32) * deviation
    if len(cuts) > 0:
        result = level_of(stream_key, shape, cuts, -0.22, 0.18) * result
    return jnp.clip(result, min=-most, max=most).astype(held_as)


def setup_inputs(seed: int = 0) -> dict:
    streams_of = jax.random.split(jax.random.key(seed), 11)
    residual_in = gaussian(streams_of[0], (TOKENS, D), 0.5, 3.0, ((0, 8),))
    mix_gain = jnp.clip(1.0 + 0.18 * jax.random.normal(streams_of[1], (D,), jnp.float32), 0.1, 1.9)
    pool_weight = gaussian(streams_of[2], (C, D), (C // 4) ** -0.5, 0.5, ((1, 4),))
    pool_scale = jnp.clip(1.0 + 0.18 * jax.random.normal(streams_of[3], (D,), jnp.float32), 0.1, 1.9)
    ffn_gain = jnp.clip(1.0 + 0.18 * jax.random.normal(streams_of[4], (D,), jnp.float32), 0.1, 1.9)
    route_ids_keys = jax.random.split(jax.random.fold_in(streams_of[5], 1), TOKENS // ROWS)
    route_ids_turns = jax.random.permutation(jax.random.fold_in(streams_of[5], 3), TOKENS // ROWS)
    route_ids = jax.vmap(lambda own, number: deal_out(jax.random.fold_in(streams_of[5], 2), own, number, ROWS, EXPERTS, TOP_K, CAP, 2))(route_ids_keys, route_ids_turns).reshape((TOKENS, TOP_K))
    route_weights = jnp.clip(jnp.exp(math.log(1.0) - 2.3025851 * jax.random.uniform(streams_of[6], (TOKENS, TOP_K), jnp.float32) ** level_of(streams_of[6], (TOKENS, TOP_K), ((0, 8),), -0.2, 0.2)), 0.1, 1.0)
    gate_weight = gaussian(streams_of[7], (EXPERTS, D, FF_EXP), D ** -0.5, 0.125, ((0, 8), (2, 4)))
    up_weight = gaussian(streams_of[8], (EXPERTS, D, FF_EXP), D ** -0.5, 0.125, ((0, 8), (2, 4)))
    down_weight = gaussian(streams_of[9], (EXPERTS, FF_EXP, D), FF_EXP ** -0.5, 0.09375, ((0, 8), (1, 4)))
    return {"residual_in": residual_in, "mix_gain": mix_gain, "pool_weight": pool_weight, "pool_scale": pool_scale, "ffn_gain": ffn_gain, "route_ids": route_ids, "route_weights": route_weights, "gate_weight": gate_weight, "up_weight": up_weight, "down_weight": down_weight}


EPS = 1e-06

def rms_scale(values, gain):
    return values * lax.rsqrt(lax.optimization_barrier(jnp.mean(values * values, axis=-1, keepdims=True)) + EPS) * gain

def reference(residual_in, mix_gain, pool_weight, pool_scale, ffn_gain, route_ids, route_weights, gate_weight, up_weight, down_weight):
    stream = residual_in.astype(jnp.float32)
    normed_in = rms_scale(stream, mix_gain).astype(jnp.bfloat16)
    shifted_in = jnp.concatenate([jnp.zeros((SPAN, D), jnp.bfloat16), normed_in], axis=0).astype(jnp.float32)
    position = jnp.arange(TOKENS, dtype=jnp.int32)
    pieces = []
    for group_index in range(GROUPS):
        window = 2 ** (group_index + 1)
        first = group_index * C
        window_sum = jnp.zeros((TOKENS, C), jnp.float32)
        for offset in range(window):
            window_sum = window_sum + shifted_in[SPAN - offset:SPAN - offset + TOKENS, first:first + C]
        divisor = jnp.minimum(position + 1, window).astype(jnp.float32)
        pieces.append(window_sum / divisor[:, None] - shifted_in[SPAN:, first:first + C])
    pooled = jnp.concatenate(pieces, axis=1).astype(jnp.bfloat16)
    mapped = jnp.concatenate([jnp.dot(pooled[:, g * C:(g + 1) * C], pool_weight[:, g * C:(g + 1) * C], preferred_element_type=jnp.float32) for g in range(GROUPS)], axis=1)
    mixer_out = (mapped * pool_scale).astype(jnp.bfloat16)
    after_mixer = (stream + mixer_out.astype(jnp.float32)).astype(jnp.bfloat16)
    normed = rms_scale(after_mixer.astype(jnp.float32), ffn_gain).astype(jnp.bfloat16)
    block_count = TOKENS // ROWS
    grouped = route_ids.reshape(block_count, ROWS * TOP_K)
    matches = (grouped[:, :, None] == jnp.arange(EXPERTS, dtype=jnp.int32)[None, None, :]).astype(jnp.int32)
    before = jnp.cumsum(matches, axis=1) - matches
    slot_of = lax.optimization_barrier(jnp.sum(before * matches, axis=-1))
    target = grouped * (block_count * CAP) + jnp.arange(block_count, dtype=jnp.int32)[:, None] * CAP + slot_of
    target = target.reshape(-1).astype(jnp.int32)
    source = (jnp.arange(TOKENS * TOP_K, dtype=jnp.int32) // TOP_K).astype(jnp.int32)
    holder = jnp.zeros((EXPERTS * block_count * CAP,), jnp.int32).at[target].set(source)
    share = FF_EXP // N_TP

    def run_expert(operands):
        indices, gate_matrix, up_matrix, down_matrix = operands
        chosen = normed[indices]
        gate_part = jnp.dot(chosen, gate_matrix, preferred_element_type=jnp.float32)
        up_part = jnp.dot(chosen, up_matrix, preferred_element_type=jnp.float32)
        hidden = (jax.nn.silu(gate_part) * up_part).astype(jnp.bfloat16)
        total = jnp.zeros((indices.shape[0], D), jnp.float32)
        for piece in range(N_TP):
            partial_value = jnp.dot(hidden[:, piece * share:(piece + 1) * share], down_matrix[piece * share:(piece + 1) * share], preferred_element_type=jnp.float32)
            total = total + partial_value.astype(jnp.bfloat16).astype(jnp.float32)
        return total.astype(jnp.bfloat16)
    outputs = lax.map(run_expert, (holder.reshape(EXPERTS, block_count * CAP), gate_weight, up_weight, down_weight))
    picked = outputs.reshape(-1, D)[target].astype(jnp.float32).reshape(TOKENS, TOP_K, D)
    expert_mix = lax.optimization_barrier(jnp.sum(route_weights[:, :, None] * picked, axis=1))
    return (after_mixer.astype(jnp.float32) + expert_mix).astype(jnp.bfloat16)
```

```python
import functools

import jax
import jax.numpy as jnp
from jax import lax
from jax.experimental import pallas as pl
from jax.experimental.pallas import tpu as pltpu
from jax.sharding import PartitionSpec as P

GROUPS = 4
SPAN = 16
TOP_K = 2
CORES = 2
SIDE = 2
EPS = 1e-06
MESH = pl.DeviceIdType.MESH
ZU, ZD, X, Y, DX, DY, FX, FY, FDX, FDY = range(10)

def from_behind(value, axis, steps):
    count = lax.axis_size(axis)
    first, last = (max(0, -steps), min(count, count - steps))
    return lax.ppermute(value, axis, [(source, source + steps) for source in range(first, last)])


def rms_scale(values, gain):
    return values * lax.rsqrt(jnp.mean(values * values, axis=-1, keepdims=True) + EPS) * gain


def slot_table(chosen_ids, experts, capacity):
    flat_ids = chosen_ids.reshape(-1)
    matches = (flat_ids[:, None] == jnp.arange(experts, dtype=jnp.int32)[None, :]).astype(jnp.int32)
    before = jnp.cumsum(matches, axis=0) - matches
    slot_of = jnp.sum(before * matches, axis=1)
    target = flat_ids * capacity + slot_of
    return (target[:, None] == jnp.arange(experts * capacity, dtype=jnp.int32)[None, :]).astype(
        jnp.float32
    )


def shards_any(
    residual_in,
    mix_gain,
    pool_weight,
    pool_scale,
    ffn_gain,
    route_ids,
    route_weights,
    gate_weight,
    up_weight,
    down_weight,
):
    tp_count = lax.axis_size("tp")
    sp_count = lax.axis_size("sp")
    tp_index = lax.axis_index("tp")
    tok_count, width = residual_in.shape
    group_width = width // GROUPS
    col_count = pool_weight.shape[1]
    row_count = tok_count // tp_count
    capacity = 2 * TOP_K * row_count // sp_count
    group_index = tp_index * col_count // group_width
    window = jnp.power(2, group_index + 1)
    stream = residual_in.astype(jnp.float32)
    inverse = lax.rsqrt(jnp.mean(stream * stream, axis=-1, keepdims=True) + EPS)
    stream_group = lax.dynamic_slice_in_dim(stream, group_index * group_width, group_width, 1)
    gain_group = lax.dynamic_slice_in_dim(mix_gain, group_index * group_width, group_width, 0)
    normed_group = (stream_group * inverse * gain_group).astype(jnp.bfloat16)
    rim_rows = from_behind(normed_group[tok_count - SPAN :], "sp", 1)
    extended = jnp.concatenate([rim_rows, normed_group], axis=0).astype(jnp.float32)
    window_sum = jnp.zeros((tok_count, group_width), jnp.float32)
    for offset in range(SPAN):
        window_sum = window_sum + jnp.where(
            offset < window, extended[SPAN - offset : SPAN - offset + tok_count], 0.0
        )
    position = lax.axis_index("sp") * tok_count + jnp.arange(tok_count, dtype=jnp.int32)
    divisor = jnp.minimum(position + 1, window).astype(jnp.float32)
    pooled = (window_sum / divisor[:, None] - extended[SPAN:]).astype(jnp.bfloat16)
    mixed = (jnp.dot(pooled, pool_weight, preferred_element_type=jnp.float32) * pool_scale).astype(
        jnp.bfloat16
    )
    stream_own = lax.dynamic_slice_in_dim(stream, tp_index * row_count, row_count, 0)
    mixed_own = lax.all_to_all(mixed, "tp", split_axis=0, concat_axis=1, tiled=True)
    after_own = (stream_own + mixed_own.astype(jnp.float32)).astype(jnp.bfloat16)
    normed_own = rms_scale(after_own.astype(jnp.float32), ffn_gain).astype(jnp.bfloat16)
    ids_own = lax.dynamic_slice_in_dim(route_ids, tp_index * row_count, row_count, 0)
    table_own = slot_table(ids_own, sp_count, capacity)
    repeated = jnp.repeat(normed_own, TOP_K, axis=0)
    outgoing = lax.dot_general(
        table_own.astype(jnp.bfloat16),
        repeated,
        (((0,), (0,)), ((), ())),
        preferred_element_type=jnp.float32,
    )
    outgoing = outgoing.astype(jnp.bfloat16).reshape(sp_count, capacity, width)
    arrived = lax.all_to_all(outgoing, "sp", split_axis=0, concat_axis=0, tiled=True)
    piece = lax.all_gather(arrived, "tp", axis=0, tiled=True)
    flat_rows = piece.reshape(-1, width)
    gate_part = jnp.dot(flat_rows, gate_weight[0], preferred_element_type=jnp.float32)
    up_part = jnp.dot(flat_rows, up_weight[0], preferred_element_type=jnp.float32)
    hidden = (jax.nn.silu(gate_part) * up_part).astype(jnp.bfloat16)
    hidden_all = hidden.reshape(piece.shape[0], piece.shape[1], hidden.shape[1])
    hidden_flat = hidden_all.reshape(-1, hidden_all.shape[-1])
    term = jnp.dot(hidden_flat, down_weight[0], preferred_element_type=jnp.float32)
    summed = lax.psum_scatter(
        term.astype(jnp.bfloat16).astype(jnp.float32).astype(jnp.bfloat16),
        "tp",
        scatter_dimension=0,
        tiled=True,
    )
    expert_out = summed.reshape(sp_count, capacity, width)
    returned_rows = lax.all_to_all(expert_out, "sp", split_axis=0, concat_axis=0, tiled=True)
    weights_own = lax.dynamic_slice_in_dim(route_weights, tp_index * row_count, row_count, 0)
    weight_table = jnp.einsum(
        "rk,rkc->rc", weights_own, table_own.reshape(row_count, TOP_K, sp_count * capacity)
    )
    expert_mix = jnp.dot(
        weight_table,
        returned_rows.reshape(-1, width).astype(jnp.float32),
        precision=lax.Precision.HIGHEST,
    )
    out_own = (after_own.astype(jnp.float32) + expert_mix).astype(jnp.bfloat16)
    return lax.all_gather(out_own, "tp", axis=0, tiled=True)


class Place:
    def __init__(self, send_sem, recv_sem):
        self.sp, self.tp = lax.axis_index("sp"), lax.axis_index("tp")
        self.levels = lax.axis_size("sp") // CORES
        self.z, self.c = self.sp // CORES, self.sp % CORES
        y, x = self.tp // SIDE, self.tp % SIDE
        self.tx = y * SIDE + (1 - x)
        self.ty = (1 - y) * SIDE + x
        self.td = (1 - y) * SIDE + (1 - x)
        self.send_sem, self.recv_sem = send_sem, recv_sem
        partner = self.z * CORES + (1 - self.c)
        self.partner = (partner, self.tp)
        self.to = {
            ZU: (self.sp + CORES, self.tp),
            ZD: (self.sp - CORES, self.tp),
            X: (self.sp, self.tx),
            Y: (self.sp, self.ty),
        }
        for kind, base in ((DX, X), (DY, Y), (FX, X), (FY, Y), (FDX, X), (FDY, Y)):
            self.to[kind] = self.to[base]

    def copy(self, kind, index, src, dst):
        return pltpu.make_async_remote_copy(
            src_ref=src,
            dst_ref=dst,
            send_sem=self.send_sem.at[kind, index],
            recv_sem=self.recv_sem.at[kind, index],
            device_id=self.to[kind],
            device_id_type=MESH,
        )

    def exists(self, offset):
        level = self.z + offset
        return (level >= 0) & (level < self.levels)

    def offsets(self):
        order = [0]
        for distance in range(1, self.levels):
            order += [-distance, distance]
        return order


def greet(place, everyone):
    barrier = pltpu.get_barrier_semaphore()

    def hello(target):
        pl.semaphore_signal(barrier, inc=1, device_id=target, device_id_type=MESH)

    hello(place.to[X])
    hello(place.to[Y])
    if everyone:
        count = lax.axis_size("sp")
        for step in range(1, count):
            hello((lax.rem(place.sp + step, count), place.tp))
        pl.semaphore_wait(barrier, count + 1)
    else:
        hello(place.partner)
        up, down = place.exists(1), place.exists(-1)
        pl.when(up)(lambda: hello(place.to[ZU]))
        pl.when(down)(lambda: hello(place.to[ZD]))
        pl.semaphore_wait(barrier, 3 + up.astype(jnp.int32) + down.astype(jnp.int32))


def gather_kernel(
    own_ref, meta_ref, out_ref, meta_out, send_sem, recv_sem, p_send, p_recv, m_send, m_recv, l_sem
):
    place = Place(send_sem, recv_sem)
    rows, cols = own_ref.shape
    half = rows // 2
    z, c, tp = place.z, place.c, place.tp
    sp_count = lax.axis_size("sp")
    tiles = SIDE * SIDE

    def block(level, core, tile, first=0, count=rows):
        start = pl.multiple_of((level * CORES + core) * rows + first, half)
        return out_ref.at[pl.ds(start, count), pl.ds(pl.multiple_of(tile * cols, cols), cols)]

    def pair_copy(level, tile, core):
        ref = block(level, core, tile)
        return pltpu.make_async_remote_copy(
            src_ref=ref,
            dst_ref=ref,
            send_sem=p_send.at[level, tile],
            recv_sem=p_recv.at[level, tile],
            device_id=place.partner,
            device_id_type=MESH,
        )

    def meta_copy(step):
        target = lax.rem(place.sp + step, sp_count)
        return pltpu.make_async_remote_copy(
            src_ref=meta_ref,
            dst_ref=meta_out.at[place.sp],
            send_sem=m_send.at[step],
            recv_sem=m_recv.at[step],
            device_id=(target, tp),
            device_id_type=MESH,
        )

    local = pltpu.make_async_copy(own_ref, block(z, c, tp), l_sem.at[0])
    local.start()
    local_meta = pltpu.make_async_copy(meta_ref, meta_out.at[place.sp], l_sem.at[1])
    local_meta.start()
    local.wait()
    local_meta.wait()
    greet(place, True)

    def whole(kind, level, tile):
        ref = block(level, c, tile)
        return place.copy(kind, level, ref, ref)

    def part(kind, level, tile):
        ref = block(level, c, tile, 0 if kind == DY else half, half)
        return place.copy(kind, level, ref, ref)

    def first(offset):
        level = z + offset
        if offset < 0:
            whole(ZU, level, tp).wait_recv()
        if offset > 0:
            whole(ZD, level, tp).wait_recv()
        if offset <= 0:
            pl.when(place.exists(1))(lambda: whole(ZU, level, tp).start())
        if offset >= 0:
            pl.when(place.exists(-1))(lambda: whole(ZD, level, tp).start())
        whole(X, level, tp).start()
        whole(Y, level, tp).start()
        pair_copy(level, tp, c).start()

    def second(offset):
        level = z + offset
        whole(X, level, place.tx).wait_recv()
        part(DY, level, place.tx).start()
        pair_copy(level, place.tx, c).start()
        whole(Y, level, place.ty).wait_recv()
        part(DX, level, place.ty).start()
        pair_copy(level, place.ty, c).start()

    def third(offset):
        level = z + offset
        part(DY, level, place.td).wait_recv()
        part(DX, level, place.td).wait_recv()
        pair_copy(level, place.td, c).start()

    order = place.offsets()
    for step in range(len(order) + 2):
        if step < len(order):
            pl.when(place.exists(order[step]))(functools.partial(first, order[step]))
        if step == 0:
            for hop in range(1, sp_count):
                meta_copy(hop).start()
        if 0 <= step - 1 < len(order):
            pl.when(place.exists(order[step - 1]))(functools.partial(second, order[step - 1]))
        if 0 <= step - 2 < len(order):
            pl.when(place.exists(order[step - 2]))(functools.partial(third, order[step - 2]))

    for hop in range(1, sp_count):
        meta_copy(hop).wait_send()
        meta_copy(hop).wait_recv()

    def sent(offset):
        level = z + offset
        if offset <= 0:
            pl.when(place.exists(1))(lambda: whole(ZU, level, tp).wait_send())
        if offset >= 0:
            pl.when(place.exists(-1))(lambda: whole(ZD, level, tp).wait_send())
        whole(X, level, tp).wait_send()
        whole(Y, level, tp).wait_send()
        part(DY, level, place.tx).wait_send()
        part(DX, level, place.ty).wait_send()

    for offset in order:
        pl.when(place.exists(offset))(functools.partial(sent, offset))
    for level in range(place.levels):
        for tile in range(tiles):
            pair_copy(level, tile, c).wait_send()
            pair_copy(level, tile, 1 - c).wait_recv()


def gather_all(own, meta, sp_count, tp_count):
    rows, cols = own.shape
    levels = sp_count // CORES
    vmem = pl.BlockSpec(memory_space=pltpu.VMEM)
    return pl.pallas_call(
        gather_kernel,
        out_shape=(
            jax.ShapeDtypeStruct((sp_count * rows, tp_count * cols), own.dtype),
            jax.ShapeDtypeStruct((sp_count,) + meta.shape, meta.dtype),
        ),
        in_specs=[vmem, vmem],
        out_specs=(vmem, vmem),
        scratch_shapes=[
            pltpu.SemaphoreType.DMA((6, levels)),
            pltpu.SemaphoreType.DMA((6, levels)),
            pltpu.SemaphoreType.DMA((levels, tp_count)),
            pltpu.SemaphoreType.DMA((levels, tp_count)),
            pltpu.SemaphoreType.DMA((sp_count,)),
            pltpu.SemaphoreType.DMA((sp_count,)),
            pltpu.SemaphoreType.DMA((2,)),
        ],
        compiler_params=pltpu.CompilerParams(collective_id=0, has_side_effects=True),
        name="gather_all",
    )(own, meta)


def combine_kernel(
    part_ref, after_ref, out_ref,
    r_pair, s_diag, r_ydiag, r_xdiag, s_x, s_y, r_x, r_y, s_z, r_up, r_down,
    send_sem, recv_sem, p_send, p_recv,
):
    place = Place(send_sem, recv_sem)
    rows, cols = after_ref.shape
    half = rows // 2
    z, c, tp = place.z, place.c, place.tp
    chunk = 32

    pl.when(z == 0)(lambda: r_up.__setitem__(Ellipsis, jnp.zeros_like(r_up)))
    pl.when(z == place.levels - 1)(lambda: r_down.__setitem__(Ellipsis, jnp.zeros_like(r_down)))
    greet(place, False)

    def pair_copy(level):
        start = pl.multiple_of((level * CORES + (1 - c)) * rows, rows)
        return pltpu.make_async_remote_copy(
            src_ref=part_ref.at[pl.ds(start, rows)],
            dst_ref=r_pair.at[level],
            send_sem=p_send.at[level],
            recv_sem=p_recv.at[level],
            device_id=place.partner,
            device_id_type=MESH,
        )

    def summed(level, tile, row, count=chunk):
        start = pl.multiple_of((level * CORES + c) * rows + row, chunk)
        lanes = pl.ds(pl.multiple_of(tile * cols, cols), cols)
        mine = part_ref[pl.ds(start, count), lanes].astype(jnp.float32)
        return mine + r_pair[level, pl.ds(pl.multiple_of(row, chunk), count), lanes].astype(
            jnp.float32
        )

    def over(first, last, body):
        def step(index, carry):
            body(pl.multiple_of(first + index * chunk, chunk))
            return carry

        lax.fori_loop(0, (last - first) // chunk, step, 0)

    def diag(kind, level):
        if kind == DY:
            return place.copy(kind, level, s_diag.at[level, pl.ds(0, half)], r_ydiag.at[level])
        return place.copy(kind, level, s_diag.at[level, pl.ds(half, half)], r_xdiag.at[level])

    def side(kind, level):
        if kind == X:
            return place.copy(kind, level, s_x.at[level], r_x.at[level])
        return place.copy(kind, level, s_y.at[level], r_y.at[level])

    def line(kind, level):
        return place.copy(kind, level, s_z.at[level], (r_up if kind == ZU else r_down).at[level])

    def first(offset):
        level = z + offset
        pair_copy(level).wait_recv()

        def body(row):
            s_diag[level, pl.ds(row, chunk)] = summed(level, place.td, row).astype(jnp.bfloat16)

        over(0, half, body)
        diag(DY, level).start()
        over(half, rows, body)
        diag(DX, level).start()

    def second(offset):
        level = z + offset

        def plain(buffer, tile):
            def body(row):
                buffer[level, pl.ds(row, chunk)] = summed(level, tile, row).astype(jnp.bfloat16)

            return body

        def joined(buffer, tile, arrived, base):
            def body(row):
                other = arrived[level, pl.ds(pl.multiple_of(row - base, chunk), chunk)]
                total = summed(level, tile, row) + other.astype(jnp.float32)
                buffer[level, pl.ds(row, chunk)] = total.astype(jnp.bfloat16)

            return body

        over(half, rows, plain(s_x, place.tx))
        over(0, half, plain(s_y, place.ty))
        diag(DY, level).wait_recv()
        over(0, half, joined(s_x, place.tx, r_ydiag, 0))
        side(X, level).start()
        diag(DX, level).wait_recv()
        over(half, rows, joined(s_y, place.ty, r_xdiag, half))
        side(Y, level).start()

    def third(offset):
        level = z + offset
        side(X, level).wait_recv()
        side(Y, level).wait_recv()
        if offset >= 0:
            pl.when(z > 0)(lambda: line(ZU, level).wait_recv())
        if offset <= 0:
            pl.when(z < place.levels - 1)(lambda: line(ZD, level).wait_recv())

        def body(row):
            at = pl.ds(row, chunk)
            total = summed(level, tp, row)
            total = total + r_x[level, at].astype(jnp.float32) + r_y[level, at].astype(jnp.float32)
            if offset >= 0:
                total = total + r_up[level, at].astype(jnp.float32)
            if offset <= 0:
                total = total + r_down[level, at].astype(jnp.float32)
            if offset == 0:
                total = total + after_ref[at].astype(jnp.float32)
                lanes = pl.ds(pl.multiple_of(tp * cols, cols), cols)
                out_ref[at, lanes] = total.astype(jnp.bfloat16)
            else:
                s_z[level, at] = total.astype(jnp.bfloat16)

        over(0, rows, body)
        if offset > 0:
            line(ZU, level).start()
        if offset < 0:
            line(ZD, level).start()

    order = place.offsets()[::-1]
    for offset in order:
        pl.when(place.exists(offset))(lambda offset=offset: pair_copy(z + offset).start())
    for step in range(len(order) + 2):
        if step < len(order):
            pl.when(place.exists(order[step]))(functools.partial(first, order[step]))
        if 0 <= step - 1 < len(order):
            pl.when(place.exists(order[step - 1]))(functools.partial(second, order[step - 1]))
        if 0 <= step - 2 < len(order):
            pl.when(place.exists(order[step - 2]))(functools.partial(third, order[step - 2]))

    def final(kind, tile):
        start, count = {FX: (0, rows), FY: (0, rows), FDY: (0, half), FDX: (half, half)}[kind]
        ref = out_ref.at[pl.ds(start, count), pl.ds(pl.multiple_of(tile * cols, cols), cols)]
        return place.copy(kind, 0, ref, ref)

    final(FX, tp).start()
    final(FY, tp).start()

    def sent(offset):
        level = z + offset
        pair_copy(level).wait_send()
        for kind in (DX, DY):
            diag(kind, level).wait_send()
        for kind in (X, Y):
            side(kind, level).wait_send()
        if offset > 0:
            line(ZU, level).wait_send()
        if offset < 0:
            line(ZD, level).wait_send()

    final(FX, place.tx).wait_recv()
    final(FDY, place.tx).start()
    final(FY, place.ty).wait_recv()
    final(FDX, place.ty).start()
    for offset in order:
        pl.when(place.exists(offset))(functools.partial(sent, offset))
    final(FDY, place.td).wait_recv()
    final(FDX, place.td).wait_recv()
    final(FX, tp).wait_send()
    final(FY, tp).wait_send()
    final(FDY, place.tx).wait_send()
    final(FDX, place.ty).wait_send()


def combine_all(parts, after, sp_count, tp_count):
    rows, cols = after.shape
    levels = sp_count // CORES
    vmem = pl.BlockSpec(memory_space=pltpu.VMEM)
    whole = pltpu.VMEM((levels, rows, cols), jnp.bfloat16)
    halved = pltpu.VMEM((levels, rows // 2, cols), jnp.bfloat16)
    return pl.pallas_call(
        combine_kernel,
        out_shape=jax.ShapeDtypeStruct((rows, tp_count * cols), after.dtype),
        in_specs=[vmem, vmem],
        out_specs=vmem,
        scratch_shapes=[
            pltpu.VMEM((levels, rows, tp_count * cols), jnp.bfloat16),
            whole, halved, halved, whole, whole, whole, whole, whole, whole, whole,
            pltpu.SemaphoreType.DMA((10, levels)),
            pltpu.SemaphoreType.DMA((10, levels)),
            pltpu.SemaphoreType.DMA((levels,)),
            pltpu.SemaphoreType.DMA((levels,)),
        ],
        compiler_params=pltpu.CompilerParams(collective_id=1, has_side_effects=True),
        name="combine_all",
    )(parts, after)


def shards(
    residual_in,
    mix_gain,
    pool_weight,
    pool_scale,
    ffn_gain,
    route_ids,
    route_weights,
    gate_weight,
    up_weight,
    down_weight,
):
    tp_count = lax.axis_size("tp")
    sp_count = lax.axis_size("sp")
    tp_index = lax.axis_index("tp")
    tok_count, width = residual_in.shape
    group_width = width // GROUPS
    col_count = pool_weight.shape[1]
    block_rows = tok_count // tp_count
    capacity = 2 * TOP_K * block_rows // sp_count
    group_index = tp_index * col_count // group_width
    window = jnp.power(2, group_index + 1)
    stream = residual_in.astype(jnp.float32)
    inverse = lax.rsqrt(jnp.mean(stream * stream, axis=-1, keepdims=True) + EPS)
    stream_group = lax.dynamic_slice_in_dim(stream, group_index * group_width, group_width, 1)
    gain_group = lax.dynamic_slice_in_dim(mix_gain, group_index * group_width, group_width, 0)
    normed_group = (stream_group * inverse * gain_group).astype(jnp.bfloat16)
    rim_rows = from_behind(normed_group[tok_count - SPAN :], "sp", 1)
    extended = jnp.concatenate([rim_rows, normed_group], axis=0).astype(jnp.float32)
    window_sum = jnp.zeros((tok_count, group_width), jnp.float32)
    for offset in range(SPAN):
        window_sum = window_sum + jnp.where(
            offset < window, extended[SPAN - offset : SPAN - offset + tok_count], 0.0
        )
    position = lax.axis_index("sp") * tok_count + jnp.arange(tok_count, dtype=jnp.int32)
    divisor = jnp.minimum(position + 1, window).astype(jnp.float32)
    pooled = (window_sum / divisor[:, None] - extended[SPAN:]).astype(jnp.bfloat16)
    mixed = (jnp.dot(pooled, pool_weight, preferred_element_type=jnp.float32) * pool_scale).astype(
        jnp.bfloat16
    )
    stream_own = lax.dynamic_slice_in_dim(stream, tp_index * col_count, col_count, 1)
    after_own = (stream_own + mixed.astype(jnp.float32)).astype(jnp.bfloat16)

    meta = jnp.concatenate(
        [
            route_ids.astype(jnp.float32).T,
            route_weights.T,
            jnp.zeros((8 - 2 * TOP_K, tok_count), jnp.float32),
        ],
        axis=0,
    )
    after_all, meta_all = gather_all(after_own, meta, sp_count, tp_count)

    expert = lax.axis_index("sp").astype(jnp.float32)
    named = (meta_all[:, :TOP_K] == expert).astype(jnp.float32)
    match = jnp.sum(named, axis=1)
    weight = jnp.sum(named * meta_all[:, TOP_K : 2 * TOP_K], axis=1)
    at = jnp.arange(tok_count, dtype=jnp.int32)
    earlier = (at[:, None] < at[None, :]) & (at[:, None] // block_rows == at[None, :] // block_rows)
    before = jnp.dot(
        match.astype(jnp.bfloat16),
        earlier.astype(jnp.bfloat16),
        preferred_element_type=jnp.float32,
    )
    slots = capacity * tp_count
    slot_of = before + (at // block_rows * capacity).astype(jnp.float32)[None, :]
    slot_of = jnp.where(match > 0, slot_of, -1.0)
    chosen = slot_of[:, None, :] == jnp.arange(slots, dtype=jnp.float32)[None, :, None]
    table = chosen.astype(jnp.bfloat16)
    slot_weight = jnp.sum(jnp.where(chosen, weight[:, None, :], 0.0), axis=-1).reshape(-1, 1)
    picked = lax.dot_general(
        table,
        after_all.reshape(sp_count, tok_count, width),
        (((2,), (1,)), ((0,), (0,))),
        preferred_element_type=jnp.float32,
    ).reshape(-1, width)
    flat_rows = rms_scale(picked, ffn_gain).astype(jnp.bfloat16)
    gate_part = jnp.dot(flat_rows, gate_weight[0], preferred_element_type=jnp.float32)
    up_part = jnp.dot(flat_rows, up_weight[0], preferred_element_type=jnp.float32)
    hidden = (jax.nn.silu(gate_part) * up_part).astype(jnp.bfloat16)
    term = jnp.dot(hidden, down_weight[0], preferred_element_type=jnp.float32)
    term = (term * slot_weight).astype(jnp.bfloat16)
    parts = lax.dot_general(
        table,
        term.reshape(sp_count, slots, width),
        (((1,), (1,)), ((0,), (0,))),
        preferred_element_type=jnp.float32,
    ).astype(jnp.bfloat16)
    return combine_all(parts.reshape(-1, width), after_own, sp_count, tp_count)


def solution(mesh):
    placed = (
        P("sp", None),
        P(),
        P(None, "tp"),
        P("tp"),
        P(),
        P("sp", None),
        P("sp", None),
        P("sp", None, "tp"),
        P("sp", None, "tp"),
        P("sp", "tp", None),
    )
    square = mesh.shape["tp"] == SIDE * SIDE and mesh.shape["sp"] % CORES == 0
    return jax.shard_map(
        shards if square else shards_any,
        mesh=mesh,
        in_specs=placed,
        out_specs=P("sp", None),
        check_vma=False,
    )
```

```python
import functools

import jax
import jax.numpy as jnp
from jax import lax
from jax.experimental import pallas as pl
from jax.experimental.pallas import tpu as pltpu
from jax.sharding import PartitionSpec as P

GROUPS = 4
SPAN = 16
TOP_K = 2
CORES = 2
SIDE = 2
EPS = 1e-06
MESH = pl.DeviceIdType.MESH
ZU, ZD, X, Y, DX, DY, FX, FY, FDX, FDY = range(10)

def from_behind(value, axis, steps):
    count = lax.axis_size(axis)
    first, last = (max(0, -steps), min(count, count - steps))
    return lax.ppermute(value, axis, [(source, source + steps) for source in range(first, last)])


def rms_scale(values, gain):
    return values * lax.rsqrt(jnp.mean(values * values, axis=-1, keepdims=True) + EPS) * gain


def slot_table(chosen_ids, experts, capacity):
    flat_ids = chosen_ids.reshape(-1)
    matches = (flat_ids[:, None] == jnp.arange(experts, dtype=jnp.int32)[None, :]).astype(jnp.int32)
    before = jnp.cumsum(matches, axis=0) - matches
    slot_of = jnp.sum(before * matches, axis=1)
    target = flat_ids * capacity + slot_of
    return (target[:, None] == jnp.arange(experts * capacity, dtype=jnp.int32)[None, :]).astype(
        jnp.float32
    )


def shards_any(
    residual_in,
    mix_gain,
    pool_weight,
    pool_scale,
    ffn_gain,
    route_ids,
    route_weights,
    gate_weight,
    up_weight,
    down_weight,
):
    tp_count = lax.axis_size("tp")
    sp_count = lax.axis_size("sp")
    tp_index = lax.axis_index("tp")
    tok_count, width = residual_in.shape
    group_width = width // GROUPS
    col_count = pool_weight.shape[1]
    row_count = tok_count // tp_count
    capacity = 2 * TOP_K * row_count // sp_count
    group_index = tp_index * col_count // group_width
    window = jnp.power(2, group_index + 1)
    stream = residual_in.astype(jnp.float32)
    inverse = lax.rsqrt(jnp.mean(stream * stream, axis=-1, keepdims=True) + EPS)
    stream_group = lax.dynamic_slice_in_dim(stream, group_index * group_width, group_width, 1)
    gain_group = lax.dynamic_slice_in_dim(mix_gain, group_index * group_width, group_width, 0)
    normed_group = (stream_group * inverse * gain_group).astype(jnp.bfloat16)
    rim_rows = from_behind(normed_group[tok_count - SPAN :], "sp", 1)
    extended = jnp.concatenate([rim_rows, normed_group], axis=0).astype(jnp.float32)
    window_sum = jnp.zeros((tok_count, group_width), jnp.float32)
    for offset in range(SPAN):
        window_sum = window_sum + jnp.where(
            offset < window, extended[SPAN - offset : SPAN - offset + tok_count], 0.0
        )
    position = lax.axis_index("sp") * tok_count + jnp.arange(tok_count, dtype=jnp.int32)
    divisor = jnp.minimum(position + 1, window).astype(jnp.float32)
    pooled = (window_sum / divisor[:, None] - extended[SPAN:]).astype(jnp.bfloat16)
    mixed = (jnp.dot(pooled, pool_weight, preferred_element_type=jnp.float32) * pool_scale).astype(
        jnp.bfloat16
    )
    stream_own = lax.dynamic_slice_in_dim(stream, tp_index * row_count, row_count, 0)
    mixed_own = lax.all_to_all(mixed, "tp", split_axis=0, concat_axis=1, tiled=True)
    after_own = (stream_own + mixed_own.astype(jnp.float32)).astype(jnp.bfloat16)
    normed_own = rms_scale(after_own.astype(jnp.float32), ffn_gain).astype(jnp.bfloat16)
    ids_own = lax.dynamic_slice_in_dim(route_ids, tp_index * row_count, row_count, 0)
    table_own = slot_table(ids_own, sp_count, capacity)
    repeated = jnp.repeat(normed_own, TOP_K, axis=0)
    outgoing = lax.dot_general(
        table_own.astype(jnp.bfloat16),
        repeated,
        (((0,), (0,)), ((), ())),
        preferred_element_type=jnp.float32,
    )
    outgoing = outgoing.astype(jnp.bfloat16).reshape(sp_count, capacity, width)
    arrived = lax.all_to_all(outgoing, "sp", split_axis=0, concat_axis=0, tiled=True)
    piece = lax.all_gather(arrived, "tp", axis=0, tiled=True)
    flat_rows = piece.reshape(-1, width)
    gate_part = jnp.dot(flat_rows, gate_weight[0], preferred_element_type=jnp.float32)
    up_part = jnp.dot(flat_rows, up_weight[0], preferred_element_type=jnp.float32)
    hidden = (jax.nn.silu(gate_part) * up_part).astype(jnp.bfloat16)
    hidden_all = hidden.reshape(piece.shape[0], piece.shape[1], hidden.shape[1])
    hidden_flat = hidden_all.reshape(-1, hidden_all.shape[-1])
    term = jnp.dot(hidden_flat, down_weight[0], preferred_element_type=jnp.float32)
    summed = lax.psum_scatter(
        term.astype(jnp.bfloat16).astype(jnp.float32).astype(jnp.bfloat16),
        "tp",
        scatter_dimension=0,
        tiled=True,
    )
    expert_out = summed.reshape(sp_count, capacity, width)
    returned_rows = lax.all_to_all(expert_out, "sp", split_axis=0, concat_axis=0, tiled=True)
    weights_own = lax.dynamic_slice_in_dim(route_weights, tp_index * row_count, row_count, 0)
    weight_table = jnp.einsum(
        "rk,rkc->rc", weights_own, table_own.reshape(row_count, TOP_K, sp_count * capacity)
    )
    expert_mix = jnp.dot(
        weight_table,
        returned_rows.reshape(-1, width).astype(jnp.float32),
        precision=lax.Precision.HIGHEST,
    )
    out_own = (after_own.astype(jnp.float32) + expert_mix).astype(jnp.bfloat16)
    return lax.all_gather(out_own, "tp", axis=0, tiled=True)


class Place:
    def __init__(self, send_sem, recv_sem):
        self.sp, self.tp = lax.axis_index("sp"), lax.axis_index("tp")
        self.levels = lax.axis_size("sp") // CORES
        self.z, self.c = self.sp // CORES, self.sp % CORES
        y, x = self.tp // SIDE, self.tp % SIDE
        self.tx = y * SIDE + (1 - x)
        self.ty = (1 - y) * SIDE + x
        self.td = (1 - y) * SIDE + (1 - x)
        self.send_sem, self.recv_sem = send_sem, recv_sem
        partner = self.z * CORES + (1 - self.c)
        self.partner = (partner, self.tp)
        self.to = {
            ZU: (self.sp + CORES, self.tp),
            ZD: (self.sp - CORES, self.tp),
            X: (self.sp, self.tx),
            Y: (self.sp, self.ty),
        }
        for kind, base in ((DX, X), (DY, Y), (FX, X), (FY, Y), (FDX, X), (FDY, Y)):
            self.to[kind] = self.to[base]

    def copy(self, kind, index, src, dst):
        return pltpu.make_async_remote_copy(
            src_ref=src,
            dst_ref=dst,
            send_sem=self.send_sem.at[kind, index],
            recv_sem=self.recv_sem.at[kind, index],
            device_id=self.to[kind],
            device_id_type=MESH,
        )

    def exists(self, offset):
        level = self.z + offset
        return (level >= 0) & (level < self.levels)

    def offsets(self):
        order = [0]
        for distance in range(1, self.levels):
            order += [-distance, distance]
        return order


def greet(place, everyone):
    barrier = pltpu.get_barrier_semaphore()

    def hello(target):
        pl.semaphore_signal(barrier, inc=1, device_id=target, device_id_type=MESH)

    hello(place.to[X])
    hello(place.to[Y])
    if everyone:
        count = lax.axis_size("sp")
        for step in range(1, count):
            hello((lax.rem(place.sp + step, count), place.tp))
        pl.semaphore_wait(barrier, count + 1)
    else:
        hello(place.partner)
        up, down = place.exists(1), place.exists(-1)
        pl.when(up)(lambda: hello(place.to[ZU]))
        pl.when(down)(lambda: hello(place.to[ZD]))
        pl.semaphore_wait(barrier, 3 + up.astype(jnp.int32) + down.astype(jnp.int32))


def gather_kernel(
    own_ref, meta_ref, result_ref, meta_out,
    out_ref, send_sem, recv_sem, p_send, p_recv, m_send, m_recv, l_sem, o_sem,
):
    place = Place(send_sem, recv_sem)
    rows, cols = own_ref.shape
    half = rows // 2
    z, c, tp = place.z, place.c, place.tp
    sp_count = lax.axis_size("sp")
    tiles = SIDE * SIDE

    def block(level, core, tile, first=0, count=rows):
        start = pl.multiple_of((level * CORES + core) * rows + first, half)
        return out_ref.at[pl.ds(start, count), pl.ds(pl.multiple_of(tile * cols, cols), cols)]

    def put_out(level, tile, core):
        start = pl.multiple_of((level * CORES + core) * rows, rows)
        lanes = pl.ds(pl.multiple_of(tile * cols, cols), cols)
        return pltpu.make_async_copy(
            block(level, core, tile),
            result_ref.at[pl.ds(start, rows), lanes],
            o_sem.at[level, tile, core],
        )

    def pair_copy(level, tile, core):
        ref = block(level, core, tile)
        return pltpu.make_async_remote_copy(
            src_ref=ref,
            dst_ref=ref,
            send_sem=p_send.at[level, tile],
            recv_sem=p_recv.at[level, tile],
            device_id=place.partner,
            device_id_type=MESH,
        )

    def meta_copy(step):
        target = lax.rem(place.sp + step, sp_count)
        return pltpu.make_async_remote_copy(
            src_ref=meta_ref,
            dst_ref=meta_out.at[place.sp],
            send_sem=m_send.at[step],
            recv_sem=m_recv.at[step],
            device_id=(target, tp),
            device_id_type=MESH,
        )

    local = pltpu.make_async_copy(own_ref, block(z, c, tp), l_sem.at[0])
    local.start()
    local_meta = pltpu.make_async_copy(meta_ref, meta_out.at[place.sp], l_sem.at[1])
    local_meta.start()
    local.wait()
    local_meta.wait()
    greet(place, True)

    def whole(kind, level, tile):
        ref = block(level, c, tile)
        return place.copy(kind, level, ref, ref)

    def part(kind, level, tile):
        ref = block(level, c, tile, 0 if kind == DY else half, half)
        return place.copy(kind, level, ref, ref)

    def first(offset):
        level = z + offset
        if offset < 0:
            whole(ZU, level, tp).wait_recv()
        if offset > 0:
            whole(ZD, level, tp).wait_recv()
        if offset <= 0:
            pl.when(place.exists(1))(lambda: whole(ZU, level, tp).start())
        if offset >= 0:
            pl.when(place.exists(-1))(lambda: whole(ZD, level, tp).start())
        whole(X, level, tp).start()
        whole(Y, level, tp).start()
        pair_copy(level, tp, c).start()
        put_out(level, tp, c).start()

    def second(offset):
        level = z + offset
        whole(X, level, place.tx).wait_recv()
        part(DY, level, place.tx).start()
        pair_copy(level, place.tx, c).start()
        put_out(level, place.tx, c).start()
        whole(Y, level, place.ty).wait_recv()
        part(DX, level, place.ty).start()
        pair_copy(level, place.ty, c).start()
        put_out(level, place.ty, c).start()

    def third(offset):
        level = z + offset
        part(DY, level, place.td).wait_recv()
        part(DX, level, place.td).wait_recv()
        pair_copy(level, place.td, c).start()
        put_out(level, place.td, c).start()

    order = place.offsets()
    stages = ((first, 0), (second, 1), (third, 2))
    for step in range(place.levels + 2):
        for stage, lag in stages:
            for offset in order:
                if abs(offset) == step - lag:
                    pl.when(place.exists(offset))(functools.partial(stage, offset))
        if step == 0:
            for hop in range(1, sp_count):
                meta_copy(hop).start()

    pairs = [(level, tile) for level in range(place.levels) for tile in range(tiles)]
    for level, tile in pairs:
        pair_copy(level, tile, 1 - c).wait_recv()
        put_out(level, tile, 1 - c).start()
    for hop in range(1, sp_count):
        meta_copy(hop).wait_send()
        meta_copy(hop).wait_recv()

    def sent(offset):
        level = z + offset
        if offset <= 0:
            pl.when(place.exists(1))(lambda: whole(ZU, level, tp).wait_send())
        if offset >= 0:
            pl.when(place.exists(-1))(lambda: whole(ZD, level, tp).wait_send())
        whole(X, level, tp).wait_send()
        whole(Y, level, tp).wait_send()
        part(DY, level, place.tx).wait_send()
        part(DX, level, place.ty).wait_send()

    for offset in order:
        pl.when(place.exists(offset))(functools.partial(sent, offset))
    for level, tile in pairs:
        pair_copy(level, tile, c).wait_send()
        put_out(level, tile, c).wait()
        put_out(level, tile, 1 - c).wait()


def gather_all(own, meta, sp_count, tp_count):
    rows, cols = own.shape
    levels = sp_count // CORES
    vmem = pl.BlockSpec(memory_space=pltpu.VMEM)
    return pl.pallas_call(
        gather_kernel,
        out_shape=(
            jax.ShapeDtypeStruct((sp_count * rows, tp_count * cols), own.dtype),
            jax.ShapeDtypeStruct((sp_count,) + meta.shape, meta.dtype),
        ),
        in_specs=[vmem, vmem],
        out_specs=(pl.BlockSpec(memory_space=pl.ANY), vmem),
        scratch_shapes=[
            pltpu.VMEM((sp_count * rows, tp_count * cols), own.dtype),
            pltpu.SemaphoreType.DMA((6, levels)),
            pltpu.SemaphoreType.DMA((6, levels)),
            pltpu.SemaphoreType.DMA((levels, tp_count)),
            pltpu.SemaphoreType.DMA((levels, tp_count)),
            pltpu.SemaphoreType.DMA((sp_count,)),
            pltpu.SemaphoreType.DMA((sp_count,)),
            pltpu.SemaphoreType.DMA((2,)),
            pltpu.SemaphoreType.DMA((levels, tp_count, CORES)),
        ],
        compiler_params=pltpu.CompilerParams(collective_id=0, has_side_effects=True),
        name="gather_all",
    )(own, meta)


def combine_kernel(
    part_ref, after_ref, out_ref,
    own_part, r_pair, s_diag, r_ydiag, r_xdiag, s_x, s_y, r_x, r_y, s_z, r_up, r_down,
    send_sem, recv_sem, p_send, p_recv, own_sem,
):
    place = Place(send_sem, recv_sem)
    rows, cols = after_ref.shape
    half = rows // 2
    z, c, tp = place.z, place.c, place.tp
    chunk = 32

    pl.when(z == 0)(lambda: r_up.__setitem__(Ellipsis, jnp.zeros_like(r_up)))
    pl.when(z == place.levels - 1)(lambda: r_down.__setitem__(Ellipsis, jnp.zeros_like(r_down)))
    greet(place, False)

    def pair_copy(level):
        start = pl.multiple_of((level * CORES + (1 - c)) * rows, rows)
        return pltpu.make_async_remote_copy(
            src_ref=part_ref.at[pl.ds(start, rows)],
            dst_ref=r_pair.at[level],
            send_sem=p_send.at[level],
            recv_sem=p_recv.at[level],
            device_id=place.partner,
            device_id_type=MESH,
        )

    def summed(level, tile, row, count=chunk):
        at = pl.ds(pl.multiple_of(row, chunk), count)
        lanes = pl.ds(pl.multiple_of(tile * cols, cols), cols)
        mine = own_part[level, at, lanes].astype(jnp.float32)
        return mine + r_pair[level, at, lanes].astype(jnp.float32)

    def own_copy(level):
        start = pl.multiple_of((level * CORES + c) * rows, rows)
        return pltpu.make_async_copy(
            part_ref.at[pl.ds(start, rows)], own_part.at[level], own_sem.at[level]
        )

    def over(first, last, body):
        def step(index, carry):
            body(pl.multiple_of(first + index * chunk, chunk))
            return carry

        lax.fori_loop(0, (last - first) // chunk, step, 0)

    def diag(kind, level):
        if kind == DY:
            return place.copy(kind, level, s_diag.at[level, pl.ds(0, half)], r_ydiag.at[level])
        return place.copy(kind, level, s_diag.at[level, pl.ds(half, half)], r_xdiag.at[level])

    def side(kind, level):
        if kind == X:
            return place.copy(kind, level, s_x.at[level], r_x.at[level])
        return place.copy(kind, level, s_y.at[level], r_y.at[level])

    def line(kind, level):
        return place.copy(kind, level, s_z.at[level], (r_up if kind == ZU else r_down).at[level])

    def first(offset):
        level = z + offset
        pair_copy(level).wait_recv()
        own_copy(level).wait()

        def body(row):
            s_diag[level, pl.ds(row, chunk)] = summed(level, place.td, row).astype(jnp.bfloat16)

        over(0, half, body)
        diag(DY, level).start()
        over(half, rows, body)
        diag(DX, level).start()

    def second(offset):
        level = z + offset

        def plain(buffer, tile):
            def body(row):
                buffer[level, pl.ds(row, chunk)] = summed(level, tile, row).astype(jnp.bfloat16)

            return body

        def joined(buffer, tile, arrived, base):
            def body(row):
                other = arrived[level, pl.ds(pl.multiple_of(row - base, chunk), chunk)]
                total = summed(level, tile, row) + other.astype(jnp.float32)
                buffer[level, pl.ds(row, chunk)] = total.astype(jnp.bfloat16)

            return body

        over(half, rows, plain(s_x, place.tx))
        over(0, half, plain(s_y, place.ty))
        diag(DY, level).wait_recv()
        over(0, half, joined(s_x, place.tx, r_ydiag, 0))
        side(X, level).start()
        diag(DX, level).wait_recv()
        over(half, rows, joined(s_y, place.ty, r_xdiag, half))
        side(Y, level).start()

    def third(offset):
        level = z + offset
        side(X, level).wait_recv()
        side(Y, level).wait_recv()
        if offset >= 0:
            pl.when(z > 0)(lambda: line(ZU, level).wait_recv())
        if offset <= 0:
            pl.when(z < place.levels - 1)(lambda: line(ZD, level).wait_recv())

        def body(row):
            at = pl.ds(row, chunk)
            total = summed(level, tp, row)
            total = total + r_x[level, at].astype(jnp.float32) + r_y[level, at].astype(jnp.float32)
            if offset >= 0:
                total = total + r_up[level, at].astype(jnp.float32)
            if offset <= 0:
                total = total + r_down[level, at].astype(jnp.float32)
            if offset == 0:
                total = total + after_ref[at].astype(jnp.float32)
                lanes = pl.ds(pl.multiple_of(tp * cols, cols), cols)
                out_ref[at, lanes] = total.astype(jnp.bfloat16)
            else:
                s_z[level, at] = total.astype(jnp.bfloat16)

        over(0, rows, body)
        if offset > 0:
            line(ZU, level).start()
        if offset < 0:
            line(ZD, level).start()

    order = place.offsets()[::-1]
    for offset in order:
        pl.when(place.exists(offset))(lambda offset=offset: pair_copy(z + offset).start())
        pl.when(place.exists(offset))(lambda offset=offset: own_copy(z + offset).start())
    stages = ((first, 0), (second, 1), (third, 4))
    for step in range(len(order) + 4):
        for stage, lag in stages:
            if 0 <= step - lag < len(order):
                offset = order[step - lag]
                pl.when(place.exists(offset))(functools.partial(stage, offset))

    def final(kind, tile):
        start, count = {FX: (0, rows), FY: (0, rows), FDY: (0, half), FDX: (half, half)}[kind]
        ref = out_ref.at[pl.ds(start, count), pl.ds(pl.multiple_of(tile * cols, cols), cols)]
        return place.copy(kind, 0, ref, ref)

    final(FX, tp).start()
    final(FY, tp).start()

    def sent(offset):
        level = z + offset
        pair_copy(level).wait_send()
        for kind in (DX, DY):
            diag(kind, level).wait_send()
        for kind in (X, Y):
            side(kind, level).wait_send()
        if offset > 0:
            line(ZU, level).wait_send()
        if offset < 0:
            line(ZD, level).wait_send()

    final(FX, place.tx).wait_recv()
    final(FDY, place.tx).start()
    final(FY, place.ty).wait_recv()
    final(FDX, place.ty).start()
    for offset in order:
        pl.when(place.exists(offset))(functools.partial(sent, offset))
    final(FDY, place.td).wait_recv()
    final(FDX, place.td).wait_recv()
    final(FX, tp).wait_send()
    final(FY, tp).wait_send()
    final(FDY, place.tx).wait_send()
    final(FDX, place.ty).wait_send()


def combine_all(parts, after, sp_count, tp_count):
    rows, cols = after.shape
    levels = sp_count // CORES
    vmem = pl.BlockSpec(memory_space=pltpu.VMEM)
    whole = pltpu.VMEM((levels, rows, cols), jnp.bfloat16)
    halved = pltpu.VMEM((levels, rows // 2, cols), jnp.bfloat16)
    return pl.pallas_call(
        combine_kernel,
        out_shape=jax.ShapeDtypeStruct((rows, tp_count * cols), after.dtype),
        in_specs=[pl.BlockSpec(memory_space=pl.ANY), vmem],
        out_specs=vmem,
        scratch_shapes=[
            pltpu.VMEM((levels, rows, tp_count * cols), jnp.bfloat16),
            pltpu.VMEM((levels, rows, tp_count * cols), jnp.bfloat16),
            whole, halved, halved, whole, whole, whole, whole, whole, whole, whole,
            pltpu.SemaphoreType.DMA((10, levels)),
            pltpu.SemaphoreType.DMA((10, levels)),
            pltpu.SemaphoreType.DMA((levels,)),
            pltpu.SemaphoreType.DMA((levels,)),
            pltpu.SemaphoreType.DMA((levels,)),
        ],
        compiler_params=pltpu.CompilerParams(collective_id=1, has_side_effects=True),
        name="combine_all",
    )(parts, after)


def shards(
    residual_in,
    mix_gain,
    pool_weight,
    pool_scale,
    ffn_gain,
    route_ids,
    route_weights,
    gate_weight,
    up_weight,
    down_weight,
):
    tp_count = lax.axis_size("tp")
    sp_count = lax.axis_size("sp")
    tp_index = lax.axis_index("tp")
    tok_count, width = residual_in.shape
    group_width = width // GROUPS
    col_count = pool_weight.shape[1]
    block_rows = tok_count // tp_count
    capacity = 2 * TOP_K * block_rows // sp_count
    group_index = tp_index * col_count // group_width
    window = jnp.power(2, group_index + 1)
    stream = residual_in.astype(jnp.float32)
    inverse = lax.rsqrt(jnp.mean(stream * stream, axis=-1, keepdims=True) + EPS)
    stream_group = lax.dynamic_slice_in_dim(residual_in, group_index * group_width, group_width, 1)
    stream_group = stream_group.astype(jnp.float32)
    gain_group = lax.dynamic_slice_in_dim(mix_gain, group_index * group_width, group_width, 0)
    normed_group = (stream_group * inverse * gain_group).astype(jnp.bfloat16)
    rim_rows = from_behind(normed_group[tok_count - SPAN :], "sp", 1)
    extended = jnp.concatenate([rim_rows, normed_group], axis=0).astype(jnp.float32)
    window_sum = jnp.zeros((tok_count, group_width), jnp.float32)
    for offset in range(SPAN):
        window_sum = window_sum + jnp.where(
            offset < window, extended[SPAN - offset : SPAN - offset + tok_count], 0.0
        )
    position = lax.axis_index("sp") * tok_count + jnp.arange(tok_count, dtype=jnp.int32)
    divisor = jnp.minimum(position + 1, window).astype(jnp.float32)
    pooled = (window_sum / divisor[:, None] - extended[SPAN:]).astype(jnp.bfloat16)
    mixed = (jnp.dot(pooled, pool_weight, preferred_element_type=jnp.float32) * pool_scale).astype(
        jnp.bfloat16
    )
    stream_own = lax.dynamic_slice_in_dim(residual_in, tp_index * col_count, col_count, 1)
    after_own = (stream_own.astype(jnp.float32) + mixed.astype(jnp.float32)).astype(jnp.bfloat16)

    meta = jnp.concatenate(
        [
            route_ids.astype(jnp.float32).T,
            route_weights.T,
            jnp.zeros((8 - 2 * TOP_K, tok_count), jnp.float32),
        ],
        axis=0,
    )
    after_all, meta_all = gather_all(after_own, meta, sp_count, tp_count)

    expert = lax.axis_index("sp").astype(jnp.float32)
    named = (meta_all[:, :TOP_K] == expert).astype(jnp.float32)
    match = jnp.sum(named, axis=1)
    weight = jnp.sum(named * meta_all[:, TOP_K : 2 * TOP_K], axis=1)
    at = jnp.arange(tok_count, dtype=jnp.int32)
    earlier = (at[:, None] < at[None, :]) & (at[:, None] // block_rows == at[None, :] // block_rows)
    before = jnp.dot(
        match.astype(jnp.bfloat16),
        earlier.astype(jnp.bfloat16),
        preferred_element_type=jnp.float32,
    )
    slots = capacity * tp_count
    slot_of = before + (at // block_rows * capacity).astype(jnp.float32)[None, :]
    slot_of = jnp.where(match > 0, slot_of, -1.0)
    chosen = slot_of[:, None, :] == jnp.arange(slots, dtype=jnp.float32)[None, :, None]
    table = chosen.astype(jnp.bfloat16)
    slot_weight = jnp.sum(jnp.where(chosen, weight[:, None, :], 0.0), axis=-1).reshape(-1, 1)
    picked = lax.dot_general(
        table,
        after_all.reshape(sp_count, tok_count, width),
        (((2,), (1,)), ((0,), (0,))),
        preferred_element_type=jnp.float32,
    ).reshape(-1, width)
    flat_rows = rms_scale(picked, ffn_gain).astype(jnp.bfloat16)
    gate_part = jnp.dot(flat_rows, gate_weight[0], preferred_element_type=jnp.float32)
    up_part = jnp.dot(flat_rows, up_weight[0], preferred_element_type=jnp.float32)
    hidden = (jax.nn.silu(gate_part) * up_part).astype(jnp.bfloat16)
    term = jnp.dot(hidden, down_weight[0], preferred_element_type=jnp.float32)
    term = (term * slot_weight).astype(jnp.bfloat16)
    parts = lax.dot_general(
        table,
        term.reshape(sp_count, slots, width),
        (((1,), (1,)), ((0,), (0,))),
        preferred_element_type=jnp.float32,
    ).astype(jnp.bfloat16)
    return combine_all(parts.reshape(-1, width), after_own, sp_count, tp_count)


def solution(mesh):
    placed = (
        P("sp", None),
        P(),
        P(None, "tp"),
        P("tp"),
        P(),
        P("sp", None),
        P("sp", None),
        P("sp", None, "tp"),
        P("sp", None, "tp"),
        P("sp", "tp", None),
    )
    square = mesh.shape["tp"] == SIDE * SIDE and mesh.shape["sp"] % CORES == 0
    return jax.shard_map(
        shards if square else shards_any,
        mesh=mesh,
        in_specs=placed,
        out_specs=P("sp", None),
        check_vma=False,
    )
```
